32 devices in a mesh: ep: 8 (over z, x), tp: 4 (over y, core).
Axes of the slice: x: 2, y: 2, z: 4, core: 2. Of those that a mesh axis runs over, the one named last changes fastest.
Arguments:
- mixer_input: bfloat16 [4096, 2048], P('ep', 'tp'), may hold values from -6 to 6
- mixer_gain: float32 [2048], replicated, may hold values from 0.1 to 1.9
- w_query: bfloat16 [2048, 1024], P(None, 'tp'), may hold values from -0.125 to 0.125
- w_key: bfloat16 [2048, 128], replicated, may hold values from -0.125 to 0.125
- w_value: bfloat16 [2048, 128], replicated, may hold values from -0.125 to 0.125
- query_gain: float32 [64], replicated, may hold values from 0.5 to 10
- key_gain: float32 [64], replicated, may hold values from 0.5 to 10
- sink_logit: float32 [16], P('tp'), may hold values from 1 to 5
- w_output: bfloat16 [1024, 2048], P('tp'), may hold values from -0.1875 to 0.1875
- expert_input: bfloat16 [1024, 2048], P('ep'), may hold values from -6 to 6
- expert_gain: float32 [2048], replicated, may hold values from 0.1 to 1.9
- route_ids: int32 [1024, 4], P('ep'), may hold values from 0 to 7, all different within a row; in each aligned block of 128 rows (0 to 127, 128 to 255, ...) at most 128 rows name the same one
- route_weight: float32 [1024, 4], P('ep'), may hold values from 0.2 to 1.2
- expert_gate: bfloat16 [8, 2048, 2048], P('ep', None, 'tp'), may hold values from -0.125 to 0.125
- expert_up: bfloat16 [8, 2048, 2048], P('ep', None, 'tp'), may hold values from -0.125 to 0.125
- expert_down: bfloat16 [8, 2048, 2048], P('ep', None, 'tp'), may hold values from -0.125 to 0.125
- shared_gate: bfloat16 [2048, 1024], P(None, 'tp'), may hold values from -0.125 to 0.125
- shared_up: bfloat16 [2048, 1024], P(None, 'tp'), may hold values from -0.125 to 0.125
- shared_down: bfloat16 [1024, 2048], P(None, 'tp'), may hold values from -0.1875 to 0.1875
Outputs:
- mixer_output: bfloat16 [4096, 2048], P('ep', 'tp')
- expert_output: bfloat16 [1024, 2048], P('ep', 'tp')
The draws below stay inside these ranges and needn't reach their ends.
Inputs may be any that keep to these rules, and one draw needn't show every extreme that they name: `route_ids`: each row names 4 different experts. In the rows of one index of ep (aligned blocks of 128 rows) no expert is named by more than 128 rows, a bound that some block reaches.
All inputs are finite; a program needn't handle non-finite values.
Results may differ from the reference program's by a relative error of at most 0.018.
The reference program's roundings to bfloat16 on the way count: a program that leaves them out, or rounds other values in their place, can miss the bound.
Values may be sent and summed in bfloat16 or wider, within the bound.
A program may use at most 64 MiB of HBM per device.

```python
import math
import jax
import jax.numpy as jnp
import numpy as np
from jax import lax

D = 2048
HEAD = 64
Q_HEADS = 16
KV_HEADS = 2
WINDOW = 128
TOK_B = 128
TOPK = 4
FF = 2048
SHARED_FF = 1024
EXPERTS = 8
CAP = 128
TOKENS_A = 4096
TOKENS_B = 1024
N_EP = 8


def gain_draw(key):
    return jax.random.uniform(key, (HEAD,), jnp.float32, 0.6, 1.6)


def draw_query_gain(key, part):
    return gain_draw(jax.random.fold_in(key, 11))


def draw_key_gain(key, part):
    return gain_draw(jax.random.fold_in(key, 23))


def level_of(rng, extent, shards, low, largest):
    loudness = 1.0
    for position, shards_of in shards:
        steps = jax.random.uniform(jax.random.fold_in(jax.random.fold_in(rng, 6), position), (shards_of,), jnp.float32, low / len(shards), largest / len(shards))
        loudness = loudness * jnp.repeat(jnp.exp(steps), extent[position] // shards_of).reshape((-1,) + (1,) * (len(extent) - 1 - position))
    return loudness


def deal_out(stream_key, own, number, rows, count, top, most, skew):
    ranking = jax.random.permutation(stream_key, count)
    heavy_load, ordinary = portions_of(count, rows * top, most, skew, True), portions_of(count, rows * top, most, skew, False)
    places = jnp.arange(count)

    def named(sizes, rotation):
        used = int((sizes > 0).sum())
        fixed = max(1, used // 4)
        shifted = fixed + (places - fixed + rotation * (used - fixed)) % max(1, count - fixed)
        return jnp.zeros((count,), jnp.int32).at[ranking[jnp.where(places < fixed, places, shifted)]].set(jnp.asarray(sizes, jnp.int32))

    sizes = jnp.where(number % 4 == 0, named(heavy_load, number // 4), named(ordinary, number - number // 4 - 1))
    mixed = jax.random.permutation(jax.random.fold_in(own, 3), count)
    donor, taker = mixed[0:count // 2 * 2:2], mixed[1:count // 2 * 2:2]
    room = jnp.minimum(sizes[donor] - 1, most - sizes[taker]) // 2
    room = jnp.where((donor == ranking[0]) | (taker == ranking[0]) | (sizes[taker] == 0), 0, jnp.maximum(room, 0))
    shifted = jax.random.randint(jax.random.fold_in(own, 4), (count // 2,), 0, 1 << 20) % (room + 1)
    sizes = sizes.at[donor].add(-shifted).at[taker].add(shifted)
    items = jnp.searchsorted(jnp.cumsum(sizes), jnp.arange(rows * top), side="right").astype(jnp.int32)
    listing = items.reshape(top, rows).T
    listing = listing[jax.random.permutation(jax.random.fold_in(own, 1), rows)]
    rotation = jax.random.randint(jax.random.fold_in(own, 2), (rows, 1), 0, top)
    return jnp.take_along_axis(listing, (jnp.arange(top)[None, :] + rotation) % top, axis=1)


def portions_of(count, total, limit, skew, full):
    loads = [(1 << 20) // math.isqrt(grade ** skew) + 1 for grade in range(1, count + 1)]
    largest = limit if full else min(limit, max(-(-total // count), total * loads[0] // sum(loads)))
    least = 1 if total - largest >= count - 1 else 0
    holding, spare = [largest] + [least] * (count - 1), total - largest - least * (count - 1)
    while spare > 0:
        movable = [i for i in range(1, count) if holding[i] < largest] or [i for i in range(1, count) if holding[i] < limit]
        mass, remaining = sum([loads[i] for i in movable]), spare
        for i in movable:
            more = min(limit - holding[i], max(1, remaining * loads[i] // mass), spare)
            holding[i] = holding[i] + more
            spare = spare - more
    return np.array(holding)


def centred(stream_key, extent, width, bound, split=(), kind=jnp.bfloat16):
    array = jax.random.normal(stream_key, extent, jnp.float32) * width
    if len(split) > 0:
        array = level_of(stream_key, extent, split, -0.22, 0.18) * array
    return jnp.clip(array, min=-bound, max=bound).astype(kind)


def setup_inputs(seed: int = 0) -> dict:
    streams_of = jax.random.split(jax.random.key(seed), 20)
    mixer_input = centred(streams_of[0], (TOKENS_A, D), 1.0, 6.0, ((0, 8), (1, 4)))
    mixer_gain = jnp.clip(1.0 + 0.18 * jax.random.normal(streams_of[1], (D,), jnp.float32), 0.1, 1.9)
    w_query = centred(streams_of[2], (D, Q_HEADS * HEAD), D ** -0.5, 0.125, ((1, 4),))
    w_key = centred(streams_of[3], (D, KV_HEADS * HEAD), D ** -0.5, 0.125)
    w_value = centred(streams_of[4], (D, KV_HEADS * HEAD), D ** -0.5, 0.125)
    query_gain = draw_query_gain(jax.random.fold_in(streams_of[19], 71), 0)
    key_gain = draw_key_gain(jax.random.fold_in(streams_of[19], 71), 0)
    sink_logit = jnp.clip(1.0 + 4.0 * jax.random.uniform(streams_of[7], (Q_HEADS,), jnp.float32) ** level_of(streams_of[7], (Q_HEADS,), ((0, 4),), -0.2, 0.2), 1.0, 5.0)
    w_output = centred(streams_of[8], (Q_HEADS * HEAD, D), (Q_HEADS * HEAD) ** -0.5, 0.1875, ((0, 4),))
    expert_input = centred(streams_of[9], (TOKENS_B, D), 1.0, 6.0, ((0, 8),))
    expert_gain = jnp.clip(1.0 + 0.18 * jax.random.normal(streams_of[10], (D,), jnp.float32), 0.1, 1.9)
    route_ids_keys = jax.random.split(jax.random.fold_in(streams_of[11], 1), TOKENS_B // TOK_B)
    route_ids_turns = jax.random.permutation(jax.random.fold_in(streams_of[11], 3), TOKENS_B // TOK_B)
    route_ids = jax.vmap(lambda own, number: deal_out(jax.random.fold_in(streams_of[11], 2), own, number, TOK_B, EXPERTS, TOPK, CAP, 1))(route_ids_keys, route_ids_turns).reshape((TOKENS_B, TOPK))
    route_weight = jnp.clip(0.2 + 1 * jax.random.uniform(streams_of[12], (TOKENS_B, TOPK), jnp.float32) ** level_of(streams_of[12], (TOKENS_B, TOPK), ((0, 8),), -0.2, 0.2), 0.2, 1.2)
    expert_gate = centred(streams_of[13], (EXPERTS, D, FF), D ** -0.5, 0.125, ((0, 8), (2, 4)))
    expert_up = centred(streams_of[14], (EXPERTS, D, FF), D ** -0.5, 0.125, ((0, 8), (2, 4)))
    expert_down = centred(streams_of[15], (EXPERTS, FF, D), FF ** -0.5, 0.125, ((0, 8), (2, 4)))
    shared_gate = centred(streams_of[16], (D, SHARED_FF), D ** -0.5, 0.125, ((1, 4),))
    shared_up = centred(streams_of[17], (D, SHARED_FF), D ** -0.5, 0.125, ((1, 4),))
    shared_down = centred(streams_of[18], (SHARED_FF, D), SHARED_FF ** -0.5, 0.1875, ((1, 4),))
    return dict(mixer_input=mixer_input, mixer_gain=mixer_gain, w_query=w_query, w_key=w_key, w_value=w_value, query_gain=query_gain, key_gain=key_gain, sink_logit=sink_logit, w_output=w_output, expert_input=expert_input, expert_gain=expert_gain, route_ids=route_ids, route_weight=route_weight, expert_gate=expert_gate, expert_up=expert_up, expert_down=expert_down, shared_gate=shared_gate, shared_up=shared_up, shared_down=shared_down)


EPSILON = 1e-06

def head_norm(matrix, gain_vector):
    return matrix * lax.rsqrt(lax.optimization_barrier(jnp.mean(matrix * matrix, axis=-1, keepdims=True)) + EPSILON) * gain_vector

def band_attend(queries, keys_own, values_own, keys_prev, values_prev, sink_logit, first_row):
    row_count = queries.shape[0]
    head_count = queries.shape[1]
    blocks = row_count // WINDOW
    keys_all = jnp.concatenate([keys_prev, keys_own], axis=0)
    values_all = jnp.concatenate([values_prev, values_own], axis=0)
    key_band = jnp.concatenate([keys_all[:row_count].reshape(blocks, WINDOW, HEAD), keys_own.reshape(blocks, WINDOW, HEAD)], axis=1)
    value_band = jnp.concatenate([values_all[:row_count].reshape(blocks, WINDOW, HEAD), values_own.reshape(blocks, WINDOW, HEAD)], axis=1)
    query_blocks = queries.reshape(blocks, WINDOW, head_count, HEAD)
    scores = jnp.einsum('nqhd,nkd->nhqk', query_blocks.astype(jnp.float32), key_band.astype(jnp.float32)) * HEAD ** (-0.5)
    query_idx = jnp.arange(WINDOW, dtype=jnp.int32)[:, None]
    key_idx = jnp.arange(2 * WINDOW, dtype=jnp.int32)[None, :]
    relative = query_idx + WINDOW - key_idx
    block_idx = jnp.arange(blocks, dtype=jnp.int32)[:, None, None]
    key_pos = first_row + block_idx * WINDOW - WINDOW + key_idx[None]
    allowed = ((relative >= 0) & (relative < WINDOW))[None] & (key_pos >= 0)
    allowed = allowed[:, None]
    masked = jnp.where(allowed, scores, -jnp.inf)
    sink_column = sink_logit.astype(jnp.float32).reshape(1, head_count, 1, 1)
    peak_score = jnp.maximum(lax.optimization_barrier(jnp.max(masked, axis=-1, keepdims=True)), sink_column)
    exponent = jnp.exp(masked - peak_score)
    denominator = lax.optimization_barrier(jnp.sum(exponent, axis=-1, keepdims=True)) + jnp.exp(sink_column - peak_score)
    probability = (exponent / denominator).astype(jnp.bfloat16)
    mixed_rows = jnp.einsum('nhqk,nkd->nqhd', probability.astype(jnp.float32), value_band.astype(jnp.float32))
    return mixed_rows.reshape(row_count, head_count * HEAD).astype(jnp.bfloat16)

def reference(mixer_input, mixer_gain, w_query, w_key, w_value, query_gain, key_gain, sink_logit, w_output, expert_input, expert_gain, route_ids, route_weight, expert_gate, expert_up, expert_down, shared_gate, shared_up, shared_down):
    rows_float = mixer_input.astype(jnp.float32)
    scaled = (rows_float * mixer_gain).astype(jnp.bfloat16)
    inv_rms = lax.rsqrt(lax.optimization_barrier(jnp.mean(rows_float * rows_float, axis=-1, keepdims=True)) + EPSILON)
    query_raw = jnp.dot(scaled, w_query, preferred_element_type=jnp.float32)
    key_raw = jnp.dot(scaled, w_key, preferred_element_type=jnp.float32)
    value_raw = jnp.dot(scaled, w_value, preferred_element_type=jnp.float32)
    queries = head_norm(query_raw.reshape(TOKENS_A, Q_HEADS, HEAD), query_gain).astype(jnp.bfloat16)
    keys_all = head_norm(key_raw.reshape(TOKENS_A, KV_HEADS, HEAD), key_gain).astype(jnp.bfloat16)
    values_all = (value_raw * inv_rms).astype(jnp.bfloat16).reshape(TOKENS_A, KV_HEADS, HEAD)
    group_size = Q_HEADS // KV_HEADS
    zero_rows = jnp.zeros((WINDOW, HEAD), jnp.bfloat16)

    def one_head(head_index):
        kv_index = head_index // group_size
        head_query = queries[:, head_index][:, None, :]
        head_keys = keys_all[:, kv_index]
        head_values = values_all[:, kv_index]
        sink_one = sink_logit[head_index].reshape(1)
        return band_attend(head_query, head_keys, head_values, zero_rows, zero_rows, sink_one, jnp.int32(0))
    per_head = lax.map(one_head, jnp.arange(Q_HEADS, dtype=jnp.int32))
    attended = jnp.transpose(per_head, (1, 0, 2)).reshape(TOKENS_A, Q_HEADS * HEAD)
    mixer_output = jnp.dot(attended, w_output, preferred_element_type=jnp.float32).astype(jnp.bfloat16)
    expert_float = expert_input.astype(jnp.float32)
    normed = (expert_float * lax.rsqrt(lax.optimization_barrier(jnp.mean(expert_float * expert_float, axis=-1, keepdims=True)) + EPSILON) * expert_gain).astype(jnp.bfloat16)
    shared_hidden = (jax.nn.silu(jnp.dot(normed, shared_gate, preferred_element_type=jnp.float32)) * jnp.dot(normed, shared_up, preferred_element_type=jnp.float32)).astype(jnp.bfloat16)
    shared_out = jnp.dot(shared_hidden, shared_down, preferred_element_type=jnp.float32)
    ids_blocks = route_ids.reshape(N_EP, TOK_B * TOPK)
    onehot = (ids_blocks[:, :, None] == jnp.arange(EXPERTS, dtype=jnp.int32)[None, None, :]).astype(jnp.int32)
    earlier = jnp.cumsum(onehot, axis=1) - onehot
    slot_index = lax.optimization_barrier(jnp.sum(earlier * onehot, axis=-1))
    block_ids = jnp.arange(N_EP, dtype=jnp.int32)[:, None]
    slot_column = (block_ids * CAP + slot_index).astype(jnp.int32)
    token_ids = (block_ids * TOK_B + jnp.arange(TOK_B * TOPK, dtype=jnp.int32)[None] // TOPK).astype(jnp.int32)
    slot_table = jnp.full((EXPERTS, N_EP * CAP), TOKENS_B, jnp.int32).at[ids_blocks, slot_column].set(token_ids)
    padded = jnp.concatenate([normed, jnp.zeros((1, D), jnp.bfloat16)], axis=0)

    def one_expert(expert_index):
        chosen = padded[slot_table[expert_index]]
        gate_pre = jnp.dot(chosen, expert_gate[expert_index], preferred_element_type=jnp.float32)
        up_pre = jnp.dot(chosen, expert_up[expert_index], preferred_element_type=jnp.float32)
        hidden = (jax.nn.silu(gate_pre) * up_pre).astype(jnp.bfloat16)
        return jnp.dot(hidden, expert_down[expert_index], preferred_element_type=jnp.float32).astype(jnp.bfloat16)
    routed = lax.map(one_expert, jnp.arange(EXPERTS, dtype=jnp.int32))
    picked = routed[ids_blocks, slot_column].reshape(TOKENS_B, TOPK, D).astype(jnp.float32)
    expert_output = (shared_out + lax.optimization_barrier(jnp.sum(picked * route_weight[:, :, None], axis=1))).astype(jnp.bfloat16)
    return (mixer_output, expert_output)
```

```python
import functools

import jax
import jax.numpy as jnp
from jax import lax
from jax.experimental import pallas as pl
from jax.experimental.pallas import tpu as pltpu
from jax.sharding import PartitionSpec as P

D = 2048
HEAD = 64
KV_HEADS = 2
WINDOW = 128
TOPK = 4


EPSILON = 1e-06


def from_behind(value, axis, steps):
    count = lax.axis_size(axis)
    first, last = (max(0, -steps), min(count, count - steps))
    return lax.ppermute(value, axis, [(source, source + steps) for source in range(first, last)])


def head_norm(matrix, gain_vector):
    return (
        matrix
        * lax.rsqrt(jnp.mean(matrix * matrix, axis=-1, keepdims=True) + EPSILON)
        * gain_vector
    )


def band_attend(queries, keys_own, values_own, keys_prev, values_prev, sink_logit, first_row):
    row_count = queries.shape[0]
    head_count = queries.shape[1]
    blocks = row_count // WINDOW
    keys_all = jnp.concatenate([keys_prev, keys_own], axis=0)
    values_all = jnp.concatenate([values_prev, values_own], axis=0)
    key_band = jnp.concatenate(
        [
            keys_all[:row_count].reshape(blocks, WINDOW, HEAD),
            keys_own.reshape(blocks, WINDOW, HEAD),
        ],
        axis=1,
    )
    value_band = jnp.concatenate(
        [
            values_all[:row_count].reshape(blocks, WINDOW, HEAD),
            values_own.reshape(blocks, WINDOW, HEAD),
        ],
        axis=1,
    )
    query_blocks = queries.reshape(blocks, WINDOW, head_count, HEAD)
    scores = jnp.einsum(
        "nqhd,nkd->nhqk", query_blocks, key_band, preferred_element_type=jnp.float32
    ) * HEAD ** (-0.5)
    query_idx = jnp.arange(WINDOW, dtype=jnp.int32)[:, None]
    key_idx = jnp.arange(2 * WINDOW, dtype=jnp.int32)[None, :]
    relative = query_idx + WINDOW - key_idx
    block_idx = jnp.arange(blocks, dtype=jnp.int32)[:, None, None]
    key_pos = first_row + block_idx * WINDOW - WINDOW + key_idx[None]
    allowed = ((relative >= 0) & (relative < WINDOW))[None] & (key_pos >= 0)
    allowed = allowed[:, None]
    masked = jnp.where(allowed, scores, -jnp.inf)
    sink_column = sink_logit.reshape(1, head_count, 1, 1)
    peak_score = jnp.maximum(jnp.max(masked, axis=-1, keepdims=True), sink_column)
    exponent = jnp.exp(masked - peak_score)
    denominator = jnp.sum(exponent, axis=-1, keepdims=True) + jnp.exp(sink_column - peak_score)
    probability = (exponent / denominator).astype(jnp.bfloat16)
    mixed_rows = jnp.einsum(
        "nhqk,nkd->nqhd", probability, value_band, preferred_element_type=jnp.float32
    )
    return mixed_rows.reshape(row_count, head_count * HEAD).astype(jnp.bfloat16)


def shards_routed(
    mixer_input,
    mixer_gain,
    w_query,
    w_key,
    w_value,
    query_gain,
    key_gain,
    sink_logit,
    w_output,
    expert_input,
    expert_gain,
    route_ids,
    route_weight,
    expert_gate,
    expert_up,
    expert_down,
    shared_gate,
    shared_up,
    shared_down,
):
    tp_count = lax.axis_size("tp")
    ep_count = lax.axis_size("ep")
    rows_local = mixer_input.shape[0]
    heads_local = w_query.shape[1] // HEAD
    kv_index = lax.axis_index("tp") // (tp_count // KV_HEADS)
    key_cols = lax.dynamic_slice_in_dim(w_key, kv_index * HEAD, HEAD, 1)
    value_cols = lax.dynamic_slice_in_dim(w_value, kv_index * HEAD, HEAD, 1)
    portion_float = lax.all_gather(mixer_input, "tp", axis=1, tiled=True).astype(jnp.float32)
    scaled = (portion_float * mixer_gain).astype(jnp.bfloat16)
    query_raw = jnp.dot(scaled, w_query, preferred_element_type=jnp.float32)
    key_raw = jnp.dot(scaled, key_cols, preferred_element_type=jnp.float32)
    value_raw = jnp.dot(scaled, value_cols, preferred_element_type=jnp.float32)
    squares = jnp.sum(portion_float * portion_float, axis=1)
    inv_rms = lax.rsqrt(squares / D + EPSILON)[:, None]
    queries = head_norm(query_raw.reshape(rows_local, heads_local, HEAD), query_gain).astype(
        jnp.bfloat16
    )
    keys_own = head_norm(key_raw, key_gain).astype(jnp.bfloat16)
    values_own = (value_raw * inv_rms).astype(jnp.bfloat16)
    keys_prev, values_prev = from_behind(
        (keys_own[rows_local - WINDOW :], values_own[rows_local - WINDOW :]), "ep", 1
    )
    first_row = lax.axis_index("ep") * rows_local
    attended = band_attend(
        queries, keys_own, values_own, keys_prev, values_prev, sink_logit, first_row
    )
    head_partial = jnp.dot(attended, w_output, preferred_element_type=jnp.float32)
    mixer_output = lax.psum_scatter(
        head_partial.astype(jnp.bfloat16), "tp", scatter_dimension=1, tiled=True
    )
    tokens_local = expert_input.shape[0]
    expert_float = expert_input.astype(jnp.float32)
    normed = (
        expert_float
        * lax.rsqrt(jnp.mean(expert_float * expert_float, axis=-1, keepdims=True) + EPSILON)
        * expert_gain
    ).astype(jnp.bfloat16)
    capacity = 2 * tokens_local * TOPK // ep_count
    flat_ids = route_ids.reshape(-1)
    onehot = (flat_ids[:, None] == jnp.arange(ep_count, dtype=jnp.int32)[None, :]).astype(jnp.int32)
    earlier = jnp.cumsum(onehot, axis=0) - onehot
    slot_index = jnp.sum(earlier * onehot, axis=-1)
    slot_column = flat_ids * capacity + slot_index
    token_ids = jnp.arange(tokens_local * TOPK, dtype=jnp.int32) // TOPK
    slot_table = (
        jnp.full((ep_count * capacity,), tokens_local, jnp.int32).at[slot_column].set(token_ids)
    )
    col_width = expert_down.shape[2]
    arrived_rows = ep_count * capacity
    own_columns = lax.dynamic_slice_in_dim(normed, lax.axis_index("tp") * col_width, col_width, 1)
    padded = jnp.concatenate([own_columns, jnp.zeros((1, col_width), jnp.bfloat16)], axis=0)
    outgoing = padded[slot_table].reshape(ep_count, capacity, col_width)
    arrived = lax.all_to_all(outgoing, "ep", split_axis=0, concat_axis=0, tiled=True).reshape(
        arrived_rows, col_width
    )
    portion = lax.all_gather(arrived, "tp", axis=1, tiled=True)
    gate_part = expert_gate[0]
    up_part = expert_up[0]
    gate_pre = jnp.dot(portion, gate_part, preferred_element_type=jnp.float32)
    up_pre = jnp.dot(portion, up_part, preferred_element_type=jnp.float32)
    routed_hidden = (jax.nn.silu(gate_pre) * up_pre).astype(jnp.bfloat16)
    shared_hidden = (
        jax.nn.silu(jnp.dot(normed, shared_gate, preferred_element_type=jnp.float32))
        * jnp.dot(normed, shared_up, preferred_element_type=jnp.float32)
    ).astype(jnp.bfloat16)
    routed_part = expert_down[0]
    routed_sum = jnp.dot(
        lax.all_gather(routed_hidden, "tp", axis=1, tiled=True),
        routed_part,
        preferred_element_type=jnp.float32,
    )
    shared_sum = jnp.dot(
        lax.all_gather(shared_hidden, "tp", axis=1, tiled=True),
        shared_down,
        preferred_element_type=jnp.float32,
    )
    expert_rows = routed_sum.astype(jnp.bfloat16).reshape(ep_count, capacity, col_width)
    returned = lax.all_to_all(expert_rows, "ep", split_axis=0, concat_axis=0, tiled=True).reshape(
        arrived_rows, col_width
    )
    picked = returned[slot_column].reshape(tokens_local, TOPK, col_width).astype(jnp.float32)
    expert_output = (shared_sum + jnp.sum(picked * route_weight[:, :, None], axis=1)).astype(
        jnp.bfloat16
    )
    return (mixer_output, expert_output)


CHUNKS = 2
COLUMNS_X = 2


def place_of(slot, ring):
    half = ring // 2
    return 0 if slot == 0 else 2 * slot - 1 if slot <= half else 2 * (ring - slot)


def ring_position(index, ring):
    row, side = index // COLUMNS_X, index % COLUMNS_X
    return row + side * (ring - 1 - 2 * row)


def ring_index(position, ring):
    side = position // (ring // COLUMNS_X)
    return 2 * position + side * (2 * ring - 1 - 4 * position)


def remote(source, target, send, receive, device):
    return pltpu.make_async_remote_copy(
        src_ref=source,
        dst_ref=target,
        send_sem=send,
        recv_sem=receive,
        device_id=device,
        device_id_type=pl.DeviceIdType.MESH,
    )


def greet(devices):
    barrier = pltpu.get_barrier_semaphore()
    for device in devices:
        pl.semaphore_signal(barrier, inc=1, device_id=device, device_id_type=pl.DeviceIdType.MESH)
    pl.semaphore_wait(barrier, len(devices))


def limit(direction, chunk, ring):
    return ring // 2 if direction == chunk else ring // 2 - 1


def slot_at(direction, distance, ring):
    return distance if direction == 0 else ring - distance


def gather_kernel(
    ring,
    rows_ref,
    gain_ref,
    dense_ref,
    mixer_ref,
    gate_hbm,
    up_hbm,
    shared_gate_hbm,
    shared_up_hbm,
    mixer_out,
    hidden_out,
    shared_out,
    dense_out,
    tok,
    gate_v,
    up_v,
    shared_gate_v,
    shared_up_v,
    load_sem,
    ring_send,
    ring_recv,
    sib_send,
    sib_recv,
    mix_send,
    mix_recv,
    hid_send,
    hid_recv,
    sh_send,
    sh_recv,
    dense_send,
    dense_recv,
):
    index, part = lax.axis_index("ep"), lax.axis_index("tp")
    far, core = part // 2, part % 2
    position = ring_position(index, ring)
    peers = [(ring_index((position + k) % ring, ring), part) for k in range(1, ring)]
    ahead, behind = peers[0], peers[-1]
    sibling = (index, 2 * far + 1 - core)
    across_part = 2 * (1 - far) + core
    across = (index, across_part)
    block, width = rows_ref.shape
    piece = block // CHUNKS
    half_width = width // 2
    hidden_width = gate_v.shape[1]

    loads = [
        pltpu.make_async_copy(source, target, load_sem.at[i])
        for i, (source, target) in enumerate(
            (
                (shared_gate_hbm, shared_gate_v),
                (shared_up_hbm, shared_up_v),
                (gate_hbm, gate_v),
                (up_hbm, up_v),
            )
        )
    ]
    for load in loads:
        load.start()
    value = rows_ref[...].astype(jnp.float32)
    normed = (
        value
        * lax.rsqrt(jnp.mean(value * value, axis=-1, keepdims=True) + EPSILON)
        * gain_ref[...]
    ).astype(jnp.bfloat16)
    tok[0, pl.ds(0, block), :] = normed[:, :half_width]
    tok[1, pl.ds(0, block), :] = normed[:, half_width:]

    greet(peers + [sibling, across])

    def chunk_ref(half, slot, chunk):
        start = place_of(slot, ring) * block + chunk * piece
        return tok.at[half, pl.ds(start, piece), :]

    pending = []

    def start(copy):
        copy.start()
        pending.append(copy)

    def hop(direction, distance, chunk):
        start(
            remote(
                chunk_ref(core, slot_at(direction, distance - 1, ring) % ring, chunk),
                chunk_ref(core, slot_at(direction, distance, ring), chunk),
                ring_send.at[direction, distance, chunk],
                ring_recv.at[direction, distance, chunk],
                ahead if direction == 0 else behind,
            )
        )

    for chunk in range(CHUNKS):
        for direction in range(2):
            hop(direction, 1, chunk)
    mixer_pieces = mix_send.shape[1]
    mixer_rows = mixer_ref.shape[0] // mixer_pieces
    mixer_cols = mixer_ref.shape[1]

    def mixer_slice(owner, i):
        return mixer_out.at[
            pl.ds(i * mixer_rows, mixer_rows),
            pl.ds(pl.multiple_of(owner * mixer_cols, mixer_cols), mixer_cols),
        ]

    for i in range(mixer_pieces):
        own = mixer_ref.at[pl.ds(i * mixer_rows, mixer_rows), :]
        start(remote(own, mixer_slice(part, i), mix_send.at[0, i], mix_recv.at[0, i], across))
    for i in range(mixer_pieces):
        own = mixer_ref.at[pl.ds(i * mixer_rows, mixer_rows), :]
        start(remote(own, mixer_slice(part, i), mix_send.at[1, i], mix_recv.at[1, i], sibling))
    keep = pltpu.make_async_copy(
        mixer_ref,
        mixer_out.at[:, pl.ds(pl.multiple_of(part * mixer_cols, mixer_cols), mixer_cols)],
        load_sem.at[4],
    )
    keep.start()
    for k in range(1, ring):
        start(
            remote(
                dense_ref, dense_out.at[k], dense_send.at[k], dense_recv.at[k], peers[k - 1]
            )
        )
    dense_out[0] = dense_ref[...]

    loads[0].wait()
    loads[1].wait()

    def product(first, count, weights, columns):
        low = tok[0, pl.ds(first, count), :]
        high = tok[1, pl.ds(first, count), :]
        return jnp.dot(
            low, weights[pl.ds(0, half_width), columns], preferred_element_type=jnp.float32
        ) + jnp.dot(
            high,
            weights[pl.ds(half_width, half_width), columns],
            preferred_element_type=jnp.float32,
        )

    everything = pl.ds(0, shared_gate_v.shape[1])
    shared_out[part] = (
        jax.nn.silu(product(0, block, shared_gate_v, everything))
        * product(0, block, shared_up_v, everything)
    ).astype(jnp.bfloat16)
    start(remote(shared_out.at[part], shared_out.at[part], sh_send.at[0], sh_recv.at[0], across))
    start(remote(shared_out.at[part], shared_out.at[part], sh_send.at[1], sh_recv.at[1], sibling))
    loads[2].wait()
    loads[3].wait()

    def hidden_ref(owner, slot):
        return hidden_out.at[owner, pl.ds(place_of(slot, ring) * block, block), :]

    tile = 256

    def compute(slots):
        first = min(place_of(slot, ring) for slot in slots) * block
        count = len(slots) * block

        def one(j, carry):
            columns = pl.ds(pl.multiple_of(j * tile, tile), tile)
            hidden_out[part, pl.ds(first, count), columns] = (
                jax.nn.silu(product(first, count, gate_v, columns))
                * product(first, count, up_v, columns)
            ).astype(jnp.bfloat16)
            return carry

        lax.fori_loop(0, hidden_width // tile, one, 0)
        for slot in slots:
            own = hidden_ref(part, slot)
            start(remote(own, own, hid_send.at[0, slot], hid_recv.at[0, slot], across))
            start(remote(own, own, hid_send.at[1, slot], hid_recv.at[1, slot], sibling))

    def arrive(distance):
        for chunk in range(CHUNKS):
            for direction in range(2):
                if distance > limit(direction, chunk, ring):
                    continue
                slot = slot_at(direction, distance, ring)
                here = chunk_ref(core, slot, chunk)
                remote(
                    here,
                    here,
                    ring_send.at[direction, distance, chunk],
                    ring_recv.at[direction, distance, chunk],
                    sibling,
                ).wait_recv()
                if distance < limit(direction, chunk, ring):
                    hop(direction, distance + 1, chunk)
                start(
                    remote(
                        here,
                        here,
                        sib_send.at[direction, distance, chunk],
                        sib_recv.at[direction, distance, chunk],
                        sibling,
                    )
                )

    def swapped(distance):
        for chunk in range(CHUNKS):
            for direction in range(2):
                if distance > limit(direction, chunk, ring):
                    continue
                there = chunk_ref(1 - core, slot_at(direction, distance, ring), chunk)
                remote(
                    there,
                    there,
                    sib_send.at[direction, distance, chunk],
                    sib_recv.at[direction, distance, chunk],
                    sibling,
                ).wait_recv()

    steps = ring // 2
    compute([0])
    arrive(1)
    for distance in range(1, steps + 1):
        if distance < steps:
            swapped(distance)
            compute([distance, ring - distance])
            arrive(distance + 1)
        else:
            swapped(distance)
            compute([distance])

    for i in range(mixer_pieces):
        here = mixer_slice(across_part, i)
        remote(here, here, mix_send.at[0, i], mix_recv.at[0, i], sibling).wait_recv()
        start(remote(here, here, mix_send.at[2, i], mix_recv.at[2, i], sibling))
    here = shared_out.at[across_part]
    remote(here, here, sh_send.at[0], sh_recv.at[0], sibling).wait_recv()
    start(remote(here, here, sh_send.at[2], sh_recv.at[2], sibling))
    order = [0]
    for distance in range(1, steps):
        order += [distance, ring - distance]
    order += [steps]
    for slot in order:
        here = hidden_ref(across_part, slot)
        remote(here, here, hid_send.at[0, slot], hid_recv.at[0, slot], sibling).wait_recv()
        start(remote(here, here, hid_send.at[2, slot], hid_recv.at[2, slot], sibling))

    sib_part = 2 * far + 1 - core
    corner = 2 * (1 - far) + 1 - core
    for path, owner in ((1, sib_part), (2, corner)):
        for i in range(mixer_pieces):
            here = mixer_slice(owner, i)
            remote(here, here, mix_send.at[path, i], mix_recv.at[path, i], sibling).wait_recv()
        here = shared_out.at[owner]
        remote(here, here, sh_send.at[path], sh_recv.at[path], sibling).wait_recv()
        for slot in order:
            here = hidden_ref(owner, slot)
            remote(
                here, here, hid_send.at[path, slot], hid_recv.at[path, slot], sibling
            ).wait_recv()
    for k in range(1, ring):
        here = dense_out.at[k]
        remote(here, here, dense_send.at[k], dense_recv.at[k], sibling).wait_recv()
    keep.wait()
    for copy in pending:
        copy.wait_send()


def scatter_kernel(
    ring,
    hidden_ref,
    weight_ref,
    shared_ref,
    attended_ref,
    w_out_ref,
    down_hbm,
    shared_down_hbm,
    mixer_out,
    expert_out,
    down_v,
    shared_down_v,
    mix_buf,
    mix_got,
    mix_sum,
    mix_far,
    going,
    coming,
    own_acc,
    load_sem,
    mix_send,
    mix_recv,
    ring_send,
    ring_recv,
):
    index, part = lax.axis_index("ep"), lax.axis_index("tp")
    far, core = part // 2, part % 2
    position = ring_position(index, ring)
    ahead = (ring_index((position + 1) % ring, ring), part)
    behind = (ring_index((position + ring - 1) % ring, ring), part)
    sibling = (index, 2 * far + 1 - core)
    across_part = 2 * (1 - far) + core
    across = (index, across_part)
    parts, block, shared_width = shared_ref.shape
    width = down_v.shape[1]
    inner = hidden_ref.shape[2]
    piece = block // CHUNKS
    loads = [
        pltpu.make_async_copy(down_hbm, down_v, load_sem.at[0]),
        pltpu.make_async_copy(shared_down_hbm, shared_down_v, load_sem.at[1]),
    ]
    for load in loads:
        load.start()
    pending = []

    def start(copy):
        copy.start()
        pending.append(copy)

    def head_block(owner):
        columns = pl.ds(pl.multiple_of(owner * width, width), width)
        return jnp.dot(
            attended_ref[...], w_out_ref[:, columns], preferred_element_type=jnp.float32
        ).astype(jnp.bfloat16)

    mix_buf[0] = head_block(2 * (1 - far) + 1 - core)
    mix_buf[1] = head_block(2 * far + 1 - core)
    greet([ahead, behind, sibling, across])
    for i in range(2):
        start(remote(mix_buf.at[i], mix_got.at[i], mix_send.at[i], mix_recv.at[i], sibling))
    mix_buf[2] = head_block(across_part)
    mix_buf[3] = head_block(part)

    loads[0].wait()
    steps = ring // 2

    def product(slots):
        first = min(place_of(slot, ring) for slot in slots) * block
        count = len(slots) * block
        total = jnp.dot(
            hidden_ref[0, pl.ds(first, count), :],
            down_v[pl.ds(0, inner), :],
            preferred_element_type=jnp.float32,
        )
        for owner in range(1, parts):
            total = total + jnp.dot(
                hidden_ref[owner, pl.ds(first, count), :],
                down_v[pl.ds(owner * inner, inner), :],
                preferred_element_type=jnp.float32,
            )
        rounded = total.astype(jnp.bfloat16).astype(jnp.float32)
        return rounded * weight_ref[pl.ds(first, count), :]

    def received(direction, distance, chunk):
        return coming.at[direction, distance, pl.ds(chunk * piece, piece), :]

    def wait_for(direction, distance, chunk):
        here = received(direction, distance, chunk)
        remote(
            here,
            here,
            ring_send.at[direction, distance, chunk],
            ring_recv.at[direction, distance, chunk],
            ahead,
        ).wait_recv()
        return here[...].astype(jnp.float32)

    def push(distance, values):
        for chunk in range(CHUNKS):
            for direction in range(2):
                longest = limit(direction, chunk, ring)
                if distance > longest:
                    continue
                value = values[direction][chunk * piece : (chunk + 1) * piece]
                if distance < longest:
                    value = value + wait_for(direction, distance + 1, chunk)
                rows = pl.ds(chunk * piece, piece)
                going[direction, distance, rows, :] = value.astype(jnp.bfloat16)
                start(
                    remote(
                        going.at[direction, distance, rows, :],
                        received(direction, distance, chunk),
                        ring_send.at[direction, distance, chunk],
                        ring_recv.at[direction, distance, chunk],
                        ahead if direction == 0 else behind,
                    )
                )

    farthest = product([steps])
    push(steps, (farthest, farthest))
    for i in range(2):
        remote(
            mix_got.at[i], mix_got.at[i], mix_send.at[i], mix_recv.at[i], sibling
        ).wait_recv()
    mix_sum[...] = (
        mix_buf[2].astype(jnp.float32) + mix_got[0].astype(jnp.float32)
    ).astype(jnp.bfloat16)
    start(remote(mix_sum, mix_far, mix_send.at[2], mix_recv.at[2], across))
    for distance in range(steps - 1, 0, -1):
        both = product([distance, ring - distance])
        push(distance, (both[block:], both[:block]))
    own = product([0])
    loads[1].wait()
    for owner in range(parts):
        own = own + jnp.dot(
            shared_ref[owner],
            shared_down_v[pl.ds(owner * shared_width, shared_width), :],
            preferred_element_type=jnp.float32,
        )
    own_acc[...] = own
    for chunk in range(CHUNKS):
        rows = pl.ds(chunk * piece, piece)
        expert_out[rows, :] = (
            own_acc[rows, :] + wait_for(0, 1, chunk) + wait_for(1, 1, chunk)
        ).astype(jnp.bfloat16)
    remote(mix_far, mix_far, mix_send.at[2], mix_recv.at[2], sibling).wait_recv()
    mixer_out[...] = (
        mix_buf[3].astype(jnp.float32)
        + mix_got[1].astype(jnp.float32)
        + mix_far[...].astype(jnp.float32)
    ).astype(jnp.bfloat16)
    for copy in pending:
        copy.wait_send()


def shards(
    mixer_input,
    mixer_gain,
    w_query,
    w_key,
    w_value,
    query_gain,
    key_gain,
    sink_logit,
    w_output,
    expert_input,
    expert_gain,
    route_ids,
    route_weight,
    expert_gate,
    expert_up,
    expert_down,
    shared_gate,
    shared_up,
    shared_down,
):
    ring = lax.axis_size("ep")
    parts = lax.axis_size("tp")
    rows_local, mixer_cols = mixer_input.shape
    tokens_local, width = expert_input.shape
    hidden_width = expert_gate.shape[2]
    shared_width = shared_gate.shape[1]
    out_width = expert_down.shape[2]
    half = ring // 2
    vmem = pl.BlockSpec(memory_space=pltpu.VMEM)
    hbm = pl.BlockSpec(memory_space=pl.ANY)
    bf16, f32 = jnp.bfloat16, jnp.float32
    dma = pltpu.SemaphoreType.DMA
    chosen = route_ids[:, :, None] == jnp.arange(ring, dtype=jnp.int32)
    dense = jnp.sum(jnp.where(chosen, route_weight[:, :, None], 0.0), axis=1).T
    mixer_pieces = 4
    mixer_full, hidden, shared_hidden, dense_all = pl.pallas_call(
        functools.partial(gather_kernel, ring),
        out_shape=(
            jax.ShapeDtypeStruct((rows_local, parts * mixer_cols), bf16),
            jax.ShapeDtypeStruct((parts, ring * tokens_local, hidden_width), bf16),
            jax.ShapeDtypeStruct((parts, tokens_local, shared_width), bf16),
            jax.ShapeDtypeStruct((ring, ring, tokens_local), f32),
        ),
        in_specs=[vmem] * 4 + [hbm] * 4,
        out_specs=(vmem,) * 4,
        scratch_shapes=[
            pltpu.VMEM((2, ring * tokens_local, width // 2), bf16),
            pltpu.VMEM((width, hidden_width), bf16),
            pltpu.VMEM((width, hidden_width), bf16),
            pltpu.VMEM((width, shared_width), bf16),
            pltpu.VMEM((width, shared_width), bf16),
            dma((5,)),
            dma((2, half + 1, CHUNKS)),
            dma((2, half + 1, CHUNKS)),
            dma((2, half + 1, CHUNKS)),
            dma((2, half + 1, CHUNKS)),
            dma((3, mixer_pieces)),
            dma((3, mixer_pieces)),
            dma((3, ring)),
            dma((3, ring)),
            dma((3,)),
            dma((3,)),
            dma((ring,)),
            dma((ring,)),
        ],
        compiler_params=pltpu.CompilerParams(
            collective_id=0, has_side_effects=True, vmem_limit_bytes=48 * 1024 * 1024
        ),
        name="gather",
    )(
        expert_input,
        expert_gain[None, :],
        dense,
        mixer_input,
        expert_gate[0],
        expert_up[0],
        shared_gate,
        shared_up,
    )

    heads_local = w_query.shape[1] // HEAD
    kv_index = lax.axis_index("tp") // (parts // KV_HEADS)
    key_cols = lax.dynamic_slice_in_dim(w_key, kv_index * HEAD, HEAD, 1)
    value_cols = lax.dynamic_slice_in_dim(w_value, kv_index * HEAD, HEAD, 1)
    portion_float = mixer_full.astype(jnp.float32)
    scaled = (portion_float * mixer_gain).astype(jnp.bfloat16)
    query_raw = jnp.dot(scaled, w_query, preferred_element_type=jnp.float32)
    both_raw = jnp.dot(
        scaled,
        jnp.concatenate([key_cols, value_cols], axis=1),
        preferred_element_type=jnp.float32,
    )
    squares = jnp.sum(portion_float * portion_float, axis=1)
    inv_rms = lax.rsqrt(squares / D + EPSILON)[:, None]
    queries = head_norm(query_raw.reshape(rows_local, heads_local, HEAD), query_gain).astype(
        jnp.bfloat16
    )
    keys_own = head_norm(both_raw[:, :HEAD], key_gain).astype(jnp.bfloat16)
    values_own = (both_raw[:, HEAD:] * inv_rms).astype(jnp.bfloat16)
    both_own = jnp.concatenate([keys_own, values_own], axis=1)
    both_prev = from_behind(both_own[rows_local - WINDOW :], "ep", 1)
    first_row = lax.axis_index("ep") * rows_local
    attended = band_attend(
        queries,
        keys_own,
        values_own,
        both_prev[:, :HEAD],
        both_prev[:, HEAD:],
        sink_logit,
        first_row,
    )
    weight_column = lax.dynamic_index_in_dim(
        dense_all, lax.axis_index("ep"), axis=1, keepdims=False
    )
    slots = [0] * ring
    for slot in range(ring):
        slots[place_of(slot, ring)] = slot
    weight_column = jnp.stack([weight_column[slot] for slot in slots]).reshape(-1, 1)
    mixer_output, expert_output = pl.pallas_call(
        functools.partial(scatter_kernel, ring),
        out_shape=(
            jax.ShapeDtypeStruct((rows_local, out_width), bf16),
            jax.ShapeDtypeStruct((tokens_local, out_width), bf16),
        ),
        in_specs=[vmem] * 5 + [hbm] * 2,
        out_specs=(vmem,) * 2,
        scratch_shapes=[
            pltpu.VMEM(expert_down.shape[1:], bf16),
            pltpu.VMEM(shared_down.shape, bf16),
            pltpu.VMEM((4, rows_local, out_width), bf16),
            pltpu.VMEM((2, rows_local, out_width), bf16),
            pltpu.VMEM((rows_local, out_width), bf16),
            pltpu.VMEM((rows_local, out_width), bf16),
            pltpu.VMEM((2, half + 1, tokens_local, out_width), bf16),
            pltpu.VMEM((2, half + 1, tokens_local, out_width), bf16),
            pltpu.VMEM((tokens_local, out_width), f32),
            dma((2,)),
            dma((3,)),
            dma((3,)),
            dma((2, half + 1, CHUNKS)),
            dma((2, half + 1, CHUNKS)),
        ],
        compiler_params=pltpu.CompilerParams(
            collective_id=1, has_side_effects=True, vmem_limit_bytes=48 * 1024 * 1024
        ),
        name="scatter",
    )(
        hidden,
        weight_column,
        shared_hidden,
        attended,
        w_output,
        expert_down[0],
        shared_down,
    )
    return (mixer_output, expert_output)


def plan(*arrays):
    route_ids = arrays[11]
    capacity = 2 * route_ids.size // lax.axis_size("ep")
    whole_blocks = capacity >= route_ids.shape[0]
    if whole_blocks and lax.axis_size("tp") == 4:
        return shards(*arrays)
    return shards_routed(*arrays)


def solution(mesh):
    in_specs = (
        P("ep", "tp"),
        P(),
        P(None, "tp"),
        P(),
        P(),
        P(),
        P(),
        P("tp"),
        P("tp", None),
        P("ep", None),
        P(),
        P("ep", None),
        P("ep", None),
        P("ep", None, "tp"),
        P("ep", None, "tp"),
        P("ep", None, "tp"),
        P(None, "tp"),
        P(None, "tp"),
        P(None, "tp"),
    )
    out_specs = (P("ep", "tp"), P("ep", "tp"))
    return jax.shard_map(plan, mesh=mesh, in_specs=in_specs, out_specs=out_specs, check_vma=False)
```

```python
import functools

import jax
import jax.numpy as jnp
from jax import lax
from jax.experimental import pallas as pl
from jax.experimental.pallas import tpu as pltpu
from jax.sharding import PartitionSpec as P

D = 2048
HEAD = 64
KV_HEADS = 2
WINDOW = 128
TOPK = 4


EPSILON = 1e-06


def from_behind(value, axis, steps):
    count = lax.axis_size(axis)
    first, last = (max(0, -steps), min(count, count - steps))
    return lax.ppermute(value, axis, [(source, source + steps) for source in range(first, last)])


def head_norm(matrix, gain_vector):
    return (
        matrix
        * lax.rsqrt(jnp.mean(matrix * matrix, axis=-1, keepdims=True) + EPSILON)
        * gain_vector
    )


def band_attend(queries, keys_own, values_own, keys_prev, values_prev, sink_logit, first_row):
    row_count = queries.shape[0]
    head_count = queries.shape[1]
    blocks = row_count // WINDOW
    keys_all = jnp.concatenate([keys_prev, keys_own], axis=0)
    values_all = jnp.concatenate([values_prev, values_own], axis=0)
    key_band = jnp.concatenate(
        [
            keys_all[:row_count].reshape(blocks, WINDOW, HEAD),
            keys_own.reshape(blocks, WINDOW, HEAD),
        ],
        axis=1,
    )
    value_band = jnp.concatenate(
        [
            values_all[:row_count].reshape(blocks, WINDOW, HEAD),
            values_own.reshape(blocks, WINDOW, HEAD),
        ],
        axis=1,
    )
    query_blocks = queries.reshape(blocks, WINDOW, head_count, HEAD)
    scores = jnp.einsum(
        "nqhd,nkd->nhqk", query_blocks, key_band, preferred_element_type=jnp.float32
    ) * HEAD ** (-0.5)
    query_idx = jnp.arange(WINDOW, dtype=jnp.int32)[:, None]
    key_idx = jnp.arange(2 * WINDOW, dtype=jnp.int32)[None, :]
    relative = query_idx + WINDOW - key_idx
    block_idx = jnp.arange(blocks, dtype=jnp.int32)[:, None, None]
    key_pos = first_row + block_idx * WINDOW - WINDOW + key_idx[None]
    allowed = ((relative >= 0) & (relative < WINDOW))[None] & (key_pos >= 0)
    allowed = allowed[:, None]
    masked = jnp.where(allowed, scores, -jnp.inf)
    sink_column = sink_logit.reshape(1, head_count, 1, 1)
    peak_score = jnp.maximum(jnp.max(masked, axis=-1, keepdims=True), sink_column)
    exponent = jnp.exp(masked - peak_score)
    denominator = jnp.sum(exponent, axis=-1, keepdims=True) + jnp.exp(sink_column - peak_score)
    probability = (exponent / denominator).astype(jnp.bfloat16)
    mixed_rows = jnp.einsum(
        "nhqk,nkd->nqhd", probability, value_band, preferred_element_type=jnp.float32
    )
    return mixed_rows.reshape(row_count, head_count * HEAD).astype(jnp.bfloat16)


def shards_routed(
    mixer_input,
    mixer_gain,
    w_query,
    w_key,
    w_value,
    query_gain,
    key_gain,
    sink_logit,
    w_output,
    expert_input,
    expert_gain,
    route_ids,
    route_weight,
    expert_gate,
    expert_up,
    expert_down,
    shared_gate,
    shared_up,
    shared_down,
):
    tp_count = lax.axis_size("tp")
    ep_count = lax.axis_size("ep")
    rows_local = mixer_input.shape[0]
    heads_local = w_query.shape[1] // HEAD
    kv_index = lax.axis_index("tp") // (tp_count // KV_HEADS)
    key_cols = lax.dynamic_slice_in_dim(w_key, kv_index * HEAD, HEAD, 1)
    value_cols = lax.dynamic_slice_in_dim(w_value, kv_index * HEAD, HEAD, 1)
    portion_float = lax.all_gather(mixer_input, "tp", axis=1, tiled=True).astype(jnp.float32)
    scaled = (portion_float * mixer_gain).astype(jnp.bfloat16)
    query_raw = jnp.dot(scaled, w_query, preferred_element_type=jnp.float32)
    key_raw = jnp.dot(scaled, key_cols, preferred_element_type=jnp.float32)
    value_raw = jnp.dot(scaled, value_cols, preferred_element_type=jnp.float32)
    squares = jnp.sum(portion_float * portion_float, axis=1)
    inv_rms = lax.rsqrt(squares / D + EPSILON)[:, None]
    queries = head_norm(query_raw.reshape(rows_local, heads_local, HEAD), query_gain).astype(
        jnp.bfloat16
    )
    keys_own = head_norm(key_raw, key_gain).astype(jnp.bfloat16)
    values_own = (value_raw * inv_rms).astype(jnp.bfloat16)
    keys_prev, values_prev = from_behind(
        (keys_own[rows_local - WINDOW :], values_own[rows_local - WINDOW :]), "ep", 1
    )
    first_row = lax.axis_index("ep") * rows_local
    attended = band_attend(
        queries, keys_own, values_own, keys_prev, values_prev, sink_logit, first_row
    )
    head_partial = jnp.dot(attended, w_output, preferred_element_type=jnp.float32)
    mixer_output = lax.psum_scatter(
        head_partial.astype(jnp.bfloat16), "tp", scatter_dimension=1, tiled=True
    )
    tokens_local = expert_input.shape[0]
    expert_float = expert_input.astype(jnp.float32)
    normed = (
        expert_float
        * lax.rsqrt(jnp.mean(expert_float * expert_float, axis=-1, keepdims=True) + EPSILON)
        * expert_gain
    ).astype(jnp.bfloat16)
    capacity = 2 * tokens_local * TOPK // ep_count
    flat_ids = route_ids.reshape(-1)
    onehot = (flat_ids[:, None] == jnp.arange(ep_count, dtype=jnp.int32)[None, :]).astype(jnp.int32)
    earlier = jnp.cumsum(onehot, axis=0) - onehot
    slot_index = jnp.sum(earlier * onehot, axis=-1)
    slot_column = flat_ids * capacity + slot_index
    token_ids = jnp.arange(tokens_local * TOPK, dtype=jnp.int32) // TOPK
    slot_table = (
        jnp.full((ep_count * capacity,), tokens_local, jnp.int32).at[slot_column].set(token_ids)
    )
    col_width = expert_down.shape[2]
    arrived_rows = ep_count * capacity
    own_columns = lax.dynamic_slice_in_dim(normed, lax.axis_index("tp") * col_width, col_width, 1)
    padded = jnp.concatenate([own_columns, jnp.zeros((1, col_width), jnp.bfloat16)], axis=0)
    outgoing = padded[slot_table].reshape(ep_count, capacity, col_width)
    arrived = lax.all_to_all(outgoing, "ep", split_axis=0, concat_axis=0, tiled=True).reshape(
        arrived_rows, col_width
    )
    portion = lax.all_gather(arrived, "tp", axis=1, tiled=True)
    gate_part = expert_gate[0]
    up_part = expert_up[0]
    gate_pre = jnp.dot(portion, gate_part, preferred_element_type=jnp.float32)
    up_pre = jnp.dot(portion, up_part, preferred_element_type=jnp.float32)
    routed_hidden = (jax.nn.silu(gate_pre) * up_pre).astype(jnp.bfloat16)
    shared_hidden = (
        jax.nn.silu(jnp.dot(normed, shared_gate, preferred_element_type=jnp.float32))
        * jnp.dot(normed, shared_up, preferred_element_type=jnp.float32)
    ).astype(jnp.bfloat16)
    routed_part = expert_down[0]
    routed_sum = jnp.dot(
        lax.all_gather(routed_hidden, "tp", axis=1, tiled=True),
        routed_part,
        preferred_element_type=jnp.float32,
    )
    shared_sum = jnp.dot(
        lax.all_gather(shared_hidden, "tp", axis=1, tiled=True),
        shared_down,
        preferred_element_type=jnp.float32,
    )
    expert_rows = routed_sum.astype(jnp.bfloat16).reshape(ep_count, capacity, col_width)
    returned = lax.all_to_all(expert_rows, "ep", split_axis=0, concat_axis=0, tiled=True).reshape(
        arrived_rows, col_width
    )
    picked = returned[slot_column].reshape(tokens_local, TOPK, col_width).astype(jnp.float32)
    expert_output = (shared_sum + jnp.sum(picked * route_weight[:, :, None], axis=1)).astype(
        jnp.bfloat16
    )
    return (mixer_output, expert_output)


CHUNKS = 2
COLUMNS_X = 2


def place_of(slot, ring):
    half = ring // 2
    return 0 if slot == 0 else 2 * slot - 1 if slot <= half else 2 * (ring - slot)


def ring_position(index, ring):
    row, side = index // COLUMNS_X, index % COLUMNS_X
    return row + side * (ring - 1 - 2 * row)


def ring_index(position, ring):
    side = position // (ring // COLUMNS_X)
    return 2 * position + side * (2 * ring - 1 - 4 * position)


def remote(source, target, send, receive, device):
    return pltpu.make_async_remote_copy(
        src_ref=source,
        dst_ref=target,
        send_sem=send,
        recv_sem=receive,
        device_id=device,
        device_id_type=pl.DeviceIdType.MESH,
    )


def greet(devices):
    barrier = pltpu.get_barrier_semaphore()
    for device in devices:
        pl.semaphore_signal(barrier, inc=1, device_id=device, device_id_type=pl.DeviceIdType.MESH)
    pl.semaphore_wait(barrier, len(devices))


def limit(direction, chunk, ring):
    return ring // 2 if direction == chunk else ring // 2 - 1


def slot_at(direction, distance, ring):
    return distance if direction == 0 else ring - distance


def layer_kernel(
    ring,
    rows_ref,
    gain_ref,
    dense_ref,
    mixer_ref,
    mixer_gain_ref,
    query_gain_ref,
    key_gain_ref,
    sink_ref,
    gate_hbm,
    up_hbm,
    shared_gate_hbm,
    shared_up_hbm,
    query_hbm,
    key_hbm,
    value_hbm,
    w_out_hbm,
    down_hbm,
    shared_down_hbm,
    mixer_result,
    expert_out,
    mixer_out,
    hidden_out,
    shared_out,
    dense_out,
    tok,
    gate_v,
    up_v,
    shared_gate_v,
    shared_up_v,
    query_v,
    key_v,
    value_v,
    w_out_ref,
    down_v,
    shared_down_v,
    heads_ref,
    band_ref,
    attended_ref,
    mix_buf,
    mix_got,
    mix_sum,
    mix_far,
    going,
    coming,
    own_acc,
    load_sem,
    keep_sem,
    ring_send,
    ring_recv,
    sib_send,
    sib_recv,
    mix_send,
    mix_recv,
    hid_send,
    hid_recv,
    sh_send,
    sh_recv,
    dense_send,
    dense_recv,
    halo_send,
    halo_recv,
    out_send,
    out_recv,
    back_send,
    back_recv,
):
    index, part = lax.axis_index("ep"), lax.axis_index("tp")
    far, core = part // 2, part % 2
    position = ring_position(index, ring)
    peers = [(ring_index((position + k) % ring, ring), part) for k in range(1, ring)]
    ahead, behind = peers[0], peers[-1]
    sibling = (index, 2 * far + 1 - core)
    across_part = 2 * (1 - far) + core
    across = (index, across_part)
    block, width = rows_ref.shape
    piece = block // CHUNKS
    half_width = width // 2
    hidden_width = gate_v.shape[1]

    loads = [
        pltpu.make_async_copy(source, target, load_sem.at[i])
        for i, (source, target) in enumerate(
            (
                (shared_gate_hbm, shared_gate_v),
                (shared_up_hbm, shared_up_v),
                (gate_hbm, gate_v),
                (up_hbm, up_v),
                (query_hbm, query_v),
                (key_hbm, key_v),
                (value_hbm, value_v),
                (w_out_hbm, w_out_ref),
                (down_hbm, down_v),
                (shared_down_hbm, shared_down_v),
            )
        )
    ]
    for load in loads:
        load.start()
    value = rows_ref[...].astype(jnp.float32)
    normed = (
        value
        * lax.rsqrt(jnp.mean(value * value, axis=-1, keepdims=True) + EPSILON)
        * gain_ref[...]
    ).astype(jnp.bfloat16)
    tok[0, pl.ds(0, block), :] = normed[:, :half_width]
    tok[1, pl.ds(0, block), :] = normed[:, half_width:]

    greet(peers + [sibling, across])

    def chunk_ref(half, slot, chunk):
        start = place_of(slot, ring) * block + chunk * piece
        return tok.at[half, pl.ds(start, piece), :]

    pending = []

    def start(copy):
        copy.start()
        pending.append(copy)

    def hop(direction, distance, chunk):
        start(
            remote(
                chunk_ref(core, slot_at(direction, distance - 1, ring) % ring, chunk),
                chunk_ref(core, slot_at(direction, distance, ring), chunk),
                ring_send.at[direction, distance, chunk],
                ring_recv.at[direction, distance, chunk],
                ahead if direction == 0 else behind,
            )
        )

    for chunk in range(CHUNKS):
        for direction in range(2):
            hop(direction, 1, chunk)
    mixer_pieces = mix_send.shape[1]
    mixer_rows = mixer_ref.shape[0] // mixer_pieces
    mixer_cols = mixer_ref.shape[1]

    def mixer_slice(owner, i):
        return mixer_out.at[
            pl.ds(i * mixer_rows, mixer_rows),
            pl.ds(pl.multiple_of(owner * mixer_cols, mixer_cols), mixer_cols),
        ]

    for i in range(mixer_pieces):
        own = mixer_ref.at[pl.ds(i * mixer_rows, mixer_rows), :]
        start(remote(own, mixer_slice(part, i), mix_send.at[0, i], mix_recv.at[0, i], across))
    for i in range(mixer_pieces):
        own = mixer_ref.at[pl.ds(i * mixer_rows, mixer_rows), :]
        start(remote(own, mixer_slice(part, i), mix_send.at[1, i], mix_recv.at[1, i], sibling))
    keep = pltpu.make_async_copy(
        mixer_ref,
        mixer_out.at[:, pl.ds(pl.multiple_of(part * mixer_cols, mixer_cols), mixer_cols)],
        keep_sem.at[0],
    )
    keep.start()
    for k in range(1, ring):
        start(
            remote(
                dense_ref, dense_out.at[k], dense_send.at[k], dense_recv.at[k], peers[k - 1]
            )
        )
    dense_out[0] = dense_ref[...]

    loads[0].wait()
    loads[1].wait()

    def product(first, count, weights, columns):
        low = tok[0, pl.ds(first, count), :]
        high = tok[1, pl.ds(first, count), :]
        return jnp.dot(
            low, weights[pl.ds(0, half_width), columns], preferred_element_type=jnp.float32
        ) + jnp.dot(
            high,
            weights[pl.ds(half_width, half_width), columns],
            preferred_element_type=jnp.float32,
        )

    everything = pl.ds(0, shared_gate_v.shape[1])
    shared_out[part] = (
        jax.nn.silu(product(0, block, shared_gate_v, everything))
        * product(0, block, shared_up_v, everything)
    ).astype(jnp.bfloat16)
    start(remote(shared_out.at[part], shared_out.at[part], sh_send.at[0], sh_recv.at[0], across))
    start(remote(shared_out.at[part], shared_out.at[part], sh_send.at[1], sh_recv.at[1], sibling))
    loads[2].wait()
    loads[3].wait()

    def hidden_ref(owner, slot):
        return hidden_out.at[owner, pl.ds(place_of(slot, ring) * block, block), :]

    tile = 256

    def compute(slots):
        first = min(place_of(slot, ring) for slot in slots) * block
        count = len(slots) * block

        def one(j, carry):
            columns = pl.ds(pl.multiple_of(j * tile, tile), tile)
            hidden_out[part, pl.ds(first, count), columns] = (
                jax.nn.silu(product(first, count, gate_v, columns))
                * product(first, count, up_v, columns)
            ).astype(jnp.bfloat16)
            return carry

        lax.fori_loop(0, hidden_width // tile, one, 0)
        for slot in slots:
            own = hidden_ref(part, slot)
            start(remote(own, own, hid_send.at[0, slot], hid_recv.at[0, slot], across))
            start(remote(own, own, hid_send.at[1, slot], hid_recv.at[1, slot], sibling))

    def arrive(distance):
        for chunk in range(CHUNKS):
            for direction in range(2):
                if distance > limit(direction, chunk, ring):
                    continue
                slot = slot_at(direction, distance, ring)
                here = chunk_ref(core, slot, chunk)
                remote(
                    here,
                    here,
                    ring_send.at[direction, distance, chunk],
                    ring_recv.at[direction, distance, chunk],
                    sibling,
                ).wait_recv()
                if distance < limit(direction, chunk, ring):
                    hop(direction, distance + 1, chunk)
                start(
                    remote(
                        here,
                        here,
                        sib_send.at[direction, distance, chunk],
                        sib_recv.at[direction, distance, chunk],
                        sibling,
                    )
                )

    def swapped(distance):
        for chunk in range(CHUNKS):
            for direction in range(2):
                if distance > limit(direction, chunk, ring):
                    continue
                there = chunk_ref(1 - core, slot_at(direction, distance, ring), chunk)
                remote(
                    there,
                    there,
                    sib_send.at[direction, distance, chunk],
                    sib_recv.at[direction, distance, chunk],
                    sibling,
                ).wait_recv()

    def forward_mixer():
        for i in range(mixer_pieces):
            here = mixer_slice(across_part, i)
            remote(here, here, mix_send.at[0, i], mix_recv.at[0, i], sibling).wait_recv()
            start(remote(here, here, mix_send.at[2, i], mix_recv.at[2, i], sibling))

    def forward_hidden(slots):
        for slot in slots:
            here = hidden_ref(across_part, slot)
            remote(here, here, hid_send.at[0, slot], hid_recv.at[0, slot], sibling).wait_recv()
            start(remote(here, here, hid_send.at[2, slot], hid_recv.at[2, slot], sibling))

    steps = ring // 2
    compute([0])
    arrive(1)
    for distance in range(1, steps + 1):
        swapped(distance)
        if distance < steps:
            compute([distance, ring - distance])
            arrive(distance + 1)
            if distance == steps - 2:
                forward_mixer()
        else:
            compute([distance])
    order = [0]
    for distance in range(1, steps):
        order += [distance, ring - distance]
    order += [steps]
    forward_hidden(order[:3])

    sib_part = 2 * far + 1 - core
    corner = 2 * (1 - far) + 1 - core
    for path, owner in ((1, sib_part), (2, corner)):
        for i in range(mixer_pieces):
            here = mixer_slice(owner, i)
            remote(here, here, mix_send.at[path, i], mix_recv.at[path, i], sibling).wait_recv()
    keep.wait()
    for load in loads[4:8]:
        load.wait()
    rows_local = mixer_ref.shape[0]
    query_sum = key_sum = value_sum = squares = 0.0
    for owner in range(mixer_out.shape[1] // mixer_cols):
        columns = pl.ds(owner * mixer_cols, mixer_cols)
        value = mixer_out[:, columns].astype(jnp.float32)
        squares = squares + jnp.sum(value * value, axis=1, keepdims=True)
        scaled = (value * mixer_gain_ref[:, columns]).astype(jnp.bfloat16)
        query_sum = query_sum + jnp.dot(
            scaled, query_v[columns, :], preferred_element_type=jnp.float32
        )
        key_sum = key_sum + jnp.dot(
            scaled, key_v[columns, :], preferred_element_type=jnp.float32
        )
        value_sum = value_sum + jnp.dot(
            scaled, value_v[columns, :], preferred_element_type=jnp.float32
        )
    second = part // (lax.axis_size("tp") // KV_HEADS)
    key_raw = jnp.where(second == 0, key_sum[:, :HEAD], key_sum[:, HEAD:])
    value_raw = jnp.where(second == 0, value_sum[:, :HEAD], value_sum[:, HEAD:])
    band_ref[pl.ds(WINDOW, rows_local), :] = jnp.concatenate(
        [
            head_norm(key_raw, key_gain_ref[...]),
            value_raw * lax.rsqrt(squares / D + EPSILON),
        ],
        axis=1,
    ).astype(jnp.bfloat16)
    heads_local = heads_ref.shape[0]
    for head in range(heads_local):
        one_head = query_sum[:, head * HEAD : (head + 1) * HEAD]
        heads_ref[head] = head_norm(one_head, query_gain_ref[...]).astype(jnp.bfloat16)
    start(
        remote(
            band_ref.at[pl.ds(rows_local, WINDOW), :],
            band_ref.at[pl.ds(0, WINDOW), :],
            halo_send.at[0],
            halo_recv.at[0],
            ((index + 1) % ring, part),
        )
    )
    forward_hidden(order[3:5])
    halo = band_ref.at[pl.ds(0, WINDOW), :]
    remote(halo, halo, halo_send.at[0], halo_recv.at[0], sibling).wait_recv()
    query_rows = heads_local * WINDOW
    row_idx = lax.broadcasted_iota(jnp.int32, (query_rows, 2 * WINDOW), 0) % WINDOW
    key_idx = lax.broadcasted_iota(jnp.int32, (query_rows, 2 * WINDOW), 1)
    relative = row_idx + WINDOW - key_idx
    in_window = (relative >= 0) & (relative < WINDOW)

    def attend(i, carry):
        first = pl.multiple_of(i * WINDOW, WINDOW)
        block_queries = heads_ref[:, pl.ds(first, WINDOW), :].reshape(query_rows, HEAD)
        band = band_ref[pl.ds(first, 2 * WINDOW), :]
        scores = lax.dot_general(
            block_queries,
            band[:, :HEAD],
            (((1,), (1,)), ((), ())),
            preferred_element_type=jnp.float32,
        ) * HEAD ** (-0.5)
        key_pos = index * rows_local + first - WINDOW + key_idx
        masked = jnp.where(in_window & (key_pos >= 0), scores, -jnp.inf)
        sink = sink_ref[...]
        peak = jnp.maximum(jnp.max(masked, axis=-1, keepdims=True), sink)
        exponent = jnp.exp(masked - peak)
        denominator = jnp.sum(exponent, axis=-1, keepdims=True) + jnp.exp(sink - peak)
        probability = (exponent / denominator).astype(jnp.bfloat16)
        mixed = jnp.dot(probability, band[:, HEAD:], preferred_element_type=jnp.float32)
        attended_ref[pl.ds(first, WINDOW), :] = jnp.concatenate(
            [mixed[head * WINDOW : (head + 1) * WINDOW] for head in range(heads_local)], axis=1
        ).astype(jnp.bfloat16)
        return carry

    lax.fori_loop(0, rows_local // WINDOW, attend, 0)

    parts, block, shared_width = shared_out.shape
    width = down_v.shape[1]
    inner = hidden_out.shape[2]
    def head_block(owner):
        columns = pl.ds(pl.multiple_of(owner * width, width), width)
        return jnp.dot(
            attended_ref[...], w_out_ref[:, columns], preferred_element_type=jnp.float32
        ).astype(jnp.bfloat16)

    mix_buf[0] = head_block(2 * (1 - far) + 1 - core)
    mix_buf[1] = head_block(2 * far + 1 - core)
    for i in range(2):
        start(remote(mix_buf.at[i], mix_got.at[i], out_send.at[i], out_recv.at[i], sibling))
    mix_buf[2] = head_block(across_part)
    mix_buf[3] = head_block(part)

    forward_hidden(order[5:])
    here = shared_out.at[across_part]
    remote(here, here, sh_send.at[0], sh_recv.at[0], sibling).wait_recv()
    start(remote(here, here, sh_send.at[2], sh_recv.at[2], sibling))
    for peer in range(1, ring):
        here = dense_out.at[peer]
        remote(here, here, dense_send.at[peer], dense_recv.at[peer], sibling).wait_recv()
    for path, owner in ((1, sib_part), (2, corner)):
        here = shared_out.at[owner]
        remote(here, here, sh_send.at[path], sh_recv.at[path], sibling).wait_recv()
        for slot in order:
            here = hidden_ref(owner, slot)
            remote(
                here, here, hid_send.at[path, slot], hid_recv.at[path, slot], sibling
            ).wait_recv()
    loads[8].wait()
    diagonal = lax.broadcasted_iota(jnp.int32, (block, block), 0) == lax.broadcasted_iota(
        jnp.int32, (block, block), 1
    )

    def weight_column(slot):
        row = dense_out[slot, pl.ds(index, 1), :]
        return jnp.sum(jnp.where(diagonal, row, 0.0), axis=1, keepdims=True)


    def weighted(slots):
        first = min(place_of(slot, ring) for slot in slots) * block
        count = len(slots) * block
        total = jnp.dot(
            hidden_out[0, pl.ds(first, count), :],
            down_v[pl.ds(0, inner), :],
            preferred_element_type=jnp.float32,
        )
        for owner in range(1, parts):
            total = total + jnp.dot(
                hidden_out[owner, pl.ds(first, count), :],
                down_v[pl.ds(owner * inner, inner), :],
                preferred_element_type=jnp.float32,
            )
        rounded = total.astype(jnp.bfloat16).astype(jnp.float32)
        ordered = sorted(slots, key=lambda slot: place_of(slot, ring))
        return rounded * jnp.concatenate([weight_column(slot) for slot in ordered], axis=0)

    def received(direction, distance, chunk):
        return coming.at[direction, distance, pl.ds(chunk * piece, piece), :]

    def wait_for(direction, distance, chunk):
        here = received(direction, distance, chunk)
        remote(
            here,
            here,
            back_send.at[direction, distance, chunk],
            back_recv.at[direction, distance, chunk],
            ahead,
        ).wait_recv()
        return here[...].astype(jnp.float32)

    def push(distance, values):
        for chunk in range(CHUNKS):
            for direction in range(2):
                longest = limit(direction, chunk, ring)
                if distance > longest:
                    continue
                value = values[direction][chunk * piece : (chunk + 1) * piece]
                if distance < longest:
                    value = value + wait_for(direction, distance + 1, chunk)
                rows = pl.ds(chunk * piece, piece)
                going[direction, distance, rows, :] = value.astype(jnp.bfloat16)
                start(
                    remote(
                        going.at[direction, distance, rows, :],
                        received(direction, distance, chunk),
                        back_send.at[direction, distance, chunk],
                        back_recv.at[direction, distance, chunk],
                        ahead if direction == 0 else behind,
                    )
                )

    farthest = weighted([steps])
    push(steps, (farthest, farthest))
    for i in range(2):
        remote(
            mix_got.at[i], mix_got.at[i], out_send.at[i], out_recv.at[i], sibling
        ).wait_recv()
    mix_sum[...] = (
        mix_buf[2].astype(jnp.float32) + mix_got[0].astype(jnp.float32)
    ).astype(jnp.bfloat16)
    start(remote(mix_sum, mix_far, out_send.at[2], out_recv.at[2], across))
    for distance in range(steps - 1, 0, -1):
        both = weighted([distance, ring - distance])
        push(distance, (both[block:], both[:block]))
    own = weighted([0])
    loads[9].wait()
    for owner in range(parts):
        own = own + jnp.dot(
            shared_out[owner],
            shared_down_v[pl.ds(owner * shared_width, shared_width), :],
            preferred_element_type=jnp.float32,
        )
    own_acc[...] = own
    for chunk in range(CHUNKS):
        rows = pl.ds(chunk * piece, piece)
        expert_out[rows, :] = (
            own_acc[rows, :] + wait_for(0, 1, chunk) + wait_for(1, 1, chunk)
        ).astype(jnp.bfloat16)
    remote(mix_far, mix_far, out_send.at[2], out_recv.at[2], sibling).wait_recv()
    mixer_result[...] = (
        mix_buf[3].astype(jnp.float32)
        + mix_got[1].astype(jnp.float32)
        + mix_far[...].astype(jnp.float32)
    ).astype(jnp.bfloat16)
    for copy in pending:
        copy.wait_send()


def shards(
    mixer_input,
    mixer_gain,
    w_query,
    w_key,
    w_value,
    query_gain,
    key_gain,
    sink_logit,
    w_output,
    expert_input,
    expert_gain,
    route_ids,
    route_weight,
    expert_gate,
    expert_up,
    expert_down,
    shared_gate,
    shared_up,
    shared_down,
):
    ring = lax.axis_size("ep")
    parts = lax.axis_size("tp")
    rows_local, mixer_cols = mixer_input.shape
    tokens_local, width = expert_input.shape
    hidden_width = expert_gate.shape[2]
    shared_width = shared_gate.shape[1]
    out_width = expert_down.shape[2]
    half = ring // 2
    vmem = pl.BlockSpec(memory_space=pltpu.VMEM)
    hbm = pl.BlockSpec(memory_space=pl.ANY)
    bf16, f32 = jnp.bfloat16, jnp.float32
    dma = pltpu.SemaphoreType.DMA
    chosen = route_ids[:, :, None] == jnp.arange(ring, dtype=jnp.int32)
    dense = jnp.sum(jnp.where(chosen, route_weight[:, :, None], 0.0), axis=1).T
    mixer_pieces = 4
    heads_local = w_query.shape[1] // HEAD
    vm = pltpu.VMEM
    return pl.pallas_call(
        functools.partial(layer_kernel, ring),
        out_shape=(
            jax.ShapeDtypeStruct((rows_local, out_width), bf16),
            jax.ShapeDtypeStruct((tokens_local, out_width), bf16),
        ),
        in_specs=[vmem] * 8 + [hbm] * 10,
        out_specs=(vmem,) * 2,
        scratch_shapes=[
            vm((rows_local, parts * mixer_cols), bf16),
            vm((parts, ring * tokens_local, hidden_width), bf16),
            vm((parts, tokens_local, shared_width), bf16),
            vm((ring, ring, tokens_local), f32),
            vm((2, ring * tokens_local, width // 2), bf16),
            vm((width, hidden_width), bf16),
            vm((width, hidden_width), bf16),
            vm((width, shared_width), bf16),
            vm((width, shared_width), bf16),
            vm(w_query.shape, bf16),
            vm(w_key.shape, bf16),
            vm(w_value.shape, bf16),
            vm(w_output.shape, bf16),
            vm(expert_down.shape[1:], bf16),
            vm(shared_down.shape, bf16),
            vm((heads_local, rows_local, HEAD), bf16),
            vm((WINDOW + rows_local, 2 * HEAD), bf16),
            vm((rows_local, heads_local * HEAD), bf16),
            vm((4, rows_local, out_width), bf16),
            vm((2, rows_local, out_width), bf16),
            vm((rows_local, out_width), bf16),
            vm((rows_local, out_width), bf16),
            vm((2, half + 1, tokens_local, out_width), bf16),
            vm((2, half + 1, tokens_local, out_width), bf16),
            vm((tokens_local, out_width), f32),
            dma((10,)),
            dma((1,)),
            dma((2, half + 1, CHUNKS)),
            dma((2, half + 1, CHUNKS)),
            dma((2, half + 1, CHUNKS)),
            dma((2, half + 1, CHUNKS)),
            dma((3, mixer_pieces)),
            dma((3, mixer_pieces)),
            dma((3, ring)),
            dma((3, ring)),
            dma((3,)),
            dma((3,)),
            dma((ring,)),
            dma((ring,)),
            dma((1,)),
            dma((1,)),
            dma((3,)),
            dma((3,)),
            dma((2, half + 1, CHUNKS)),
            dma((2, half + 1, CHUNKS)),
        ],
        compiler_params=pltpu.CompilerParams(
            collective_id=0, has_side_effects=True, vmem_limit_bytes=62 * 1024 * 1024
        ),
        name="layer",
    )(
        expert_input,
        expert_gain[None, :],
        dense,
        mixer_input,
        mixer_gain[None, :],
        query_gain[None, :],
        key_gain[None, :],
        jnp.repeat(sink_logit, WINDOW)[:, None],
        expert_gate[0],
        expert_up[0],
        shared_gate,
        shared_up,
        w_query,
        w_key,
        w_value,
        w_output,
        expert_down[0],
        shared_down,
    )


def plan(*arrays):
    route_ids = arrays[11]
    capacity = 2 * route_ids.size // lax.axis_size("ep")
    whole_blocks = capacity >= route_ids.shape[0]
    if whole_blocks and lax.axis_size("tp") == 4:
        return shards(*arrays)
    return shards_routed(*arrays)


def solution(mesh):
    in_specs = (
        P("ep", "tp"),
        P(),
        P(None, "tp"),
        P(),
        P(),
        P(),
        P(),
        P("tp"),
        P("tp", None),
        P("ep", None),
        P(),
        P("ep", None),
        P("ep", None),
        P("ep", None, "tp"),
        P("ep", None, "tp"),
        P("ep", None, "tp"),
        P(None, "tp"),
        P(None, "tp"),
        P(None, "tp"),
    )
    out_specs = (P("ep", "tp"), P("ep", "tp"))
    return jax.shard_map(plan, mesh=mesh, in_specs=in_specs, out_specs=out_specs, check_vma=False)
```
